32 devices in a mesh: kv: 8 (over z, y), tp: 4 (over x, core).
Axes of the slice: x: 2, y: 2, z: 4, core: 2. Of those that a mesh axis runs over, the one named last changes fastest.
Arguments:
- tokens: bfloat16 [64, 6, 4096], P('kv'), may hold values from -6 to 6
- norm_gain: float32 [4096], replicated, may hold values from 0.1 to 1.9
- w_query: bfloat16 [4096, 2048], P('kv', 'tp'), may hold values from -0.09375 to 0.09375
- w_key: bfloat16 [4096, 2048], P('kv', 'tp'), may hold values from -0.09375 to 0.09375
- w_value: bfloat16 [4096, 2048], P('kv', 'tp'), may hold values from -0.09375 to 0.09375
- w_outgate: bfloat16 [4096, 2048], P('kv', 'tp'), may hold values from -0.09375 to 0.09375
- w_gates: bfloat16 [4096, 2, 16], P('kv', None, 'tp'), may hold values from -0.09375 to 0.09375
- forget_bias: float32 [16], P('tp'), may hold values from 1 to 6
- head_gain: float32 [2048], P('tp'), may hold values from 0.1 to 1.9
- w_mix: bfloat16 [2048, 4096], P('tp', 'kv'), may hold values from -0.125 to 0.125
- state_cell: float32 [64, 16, 128, 128], P('kv', 'tp'), may hold values from -4 to 4
- state_norm: float32 [64, 16, 128], P('kv', 'tp'), may hold values from -4 to 4
- state_max: float32 [64, 16], P('kv', 'tp'), may hold values from -4 to 120
- pend_keys: bfloat16 [64, 6, 2048], P('kv', None, 'tp'), may hold values from -6 to 6
- pend_values: bfloat16 [64, 6, 2048], P('kv', None, 'tp'), may hold values from -6 to 6
- pend_gates: float32 [64, 6, 2, 16], P('kv', None, None, 'tp'), may hold values from -6 to 6
- accepted: int32 [64], P('kv'), may hold values from 0 to 6
Outputs:
- mixed: bfloat16 [64, 6, 4096], P('kv', None, 'tp')
- new_cell: float32 [64, 16, 128, 128], P('kv', 'tp')
- new_norm: float32 [64, 16, 128], P('kv', 'tp')
- new_max: float32 [64, 16], P('kv', 'tp')
The draws below stay inside these ranges and needn't reach their ends.
All inputs are finite; a program needn't handle non-finite values.
Results may differ from the reference program's by a relative error of at most 0.018.
Values may be sent and summed in bfloat16 or wider, within the bound.
A program may use at most 128 MiB of HBM per device.

```python
import jax
import jax.numpy as jnp
from jax import lax

D = 4096
HEADS = 16
HD = 128
PROPS = 6
BR_W = 2048
SEQS = 64
N_TP = 4


def draw_state_max(key, part):
    return jnp.clip(1.5 * jax.random.normal(key, (SEQS, HEADS), jnp.float32), -4.0, 4.0)


def with_ends(values, rng, smallest, top_value):
    longest = values.shape.index(max(values.shape))
    spots = []
    for shift in (0, 1):
        where = [jax.random.randint(jax.random.fold_in(rng, axis), (), 0, length) for axis, length in enumerate(values.shape)]
        where[longest] = (where[longest] + shift) % values.shape[longest]
        spots.append(tuple(where))
    return values.at[spots[0]].set(smallest).at[spots[1]].set(top_value)


def levels(rng, extent, split, least, largest):
    level = 1.0
    for dim, parts in split:
        heights = jax.random.uniform(jax.random.fold_in(jax.random.fold_in(rng, 6), dim), (parts,), jnp.float32, least / len(split), largest / len(split))
        level = level * jnp.repeat(jnp.exp(heights), extent[dim] // parts).reshape((-1,) + (1,) * (len(extent) - 1 - dim))
    return level


def bell_draw(stream_key, dims, spread, most, split=(), dtype=jnp.bfloat16):
    values = jax.random.normal(stream_key, dims, jnp.float32) * spread
    if len(split) > 0:
        values = levels(stream_key, dims, split, -0.22, 0.18) * values
    return jnp.clip(values, min=-most, max=most).astype(dtype)


def setup_inputs(seed: int = 0) -> dict:
    key_list = jax.random.split(jax.random.key(seed), 18)
    return {
        "tokens": bell_draw(key_list[0], (SEQS, PROPS, D), 1.0, 6.0, ((0, 8),)),
        "norm_gain": jnp.clip(1.0 + 0.18 * jax.random.normal(key_list[1], (D,), jnp.float32), 0.1, 1.9),
        "w_query": bell_draw(key_list[2], (D, BR_W), D ** -0.5, 0.09375, ((0, 8), (1, 4))),
        "w_key": bell_draw(key_list[3], (D, BR_W), D ** -0.5, 0.09375, ((0, 8), (1, 4))),
        "w_value": bell_draw(key_list[4], (D, BR_W), D ** -0.5, 0.09375, ((0, 8), (1, 4))),
        "w_outgate": bell_draw(key_list[5], (D, BR_W), D ** -0.5, 0.09375, ((0, 8), (1, 4))),
        "w_gates": bell_draw(key_list[6], (D, 2, HEADS), D ** -0.5, 0.09375, ((0, 8), (2, 4))),
        "forget_bias": jnp.clip(1.0 + 5.0 * jax.random.uniform(key_list[7], (HEADS,), jnp.float32) ** levels(key_list[7], (HEADS,), ((0, 4),), -0.2, 0.2), 1.0, 6.0),
        "head_gain": jnp.clip(1.0 + 0.18 * jax.random.normal(key_list[8], (BR_W,), jnp.float32), 0.1, 1.9),
        "w_mix": bell_draw(key_list[9], (BR_W, D), BR_W ** -0.5, 0.125, ((0, 4), (1, 8))),
        "state_cell": bell_draw(key_list[10], (SEQS, HEADS, HD, HD), 0.3, 4.0, ((0, 8), (1, 4)), jnp.float32),
        "state_norm": bell_draw(key_list[11], (SEQS, HEADS, HD), 0.3, 4.0, ((0, 8), (1, 4)), jnp.float32),
        "state_max": draw_state_max(jax.random.fold_in(key_list[17], 71), 0),
        "pend_keys": bell_draw(key_list[13], (SEQS, PROPS, BR_W), 1.0, 6.0, ((0, 8), (2, 4))),
        "pend_values": bell_draw(key_list[14], (SEQS, PROPS, BR_W), 1.0, 6.0, ((0, 8), (2, 4))),
        "pend_gates": bell_draw(key_list[15], (SEQS, PROPS, 2, HEADS), 1.0, 6.0, ((0, 8), (3, 4)), jnp.float32),
        "accepted": with_ends(jax.random.randint(key_list[16], (SEQS,), 0, PROPS + 1), jax.random.fold_in(key_list[16], 1), 0, PROPS).astype(jnp.int32),
    }


epsilon = 1e-06
very_low = -1e+30
highest = lax.Precision.HIGHEST

def fold_pending(cell_state, normer, stabilizer, key_rows, value_rows, gate_rows, forget_shift, accepted):
    proposals = key_rows.shape[1]
    accepted_mask = jnp.arange(proposals)[None, :, None] < accepted[:, None, None]
    log_in = jnp.where(accepted_mask, gate_rows[:, :, 0, :], very_low)
    log_keep = jnp.where(accepted_mask, jax.nn.log_sigmoid(gate_rows[:, :, 1, :] + forget_shift), 0.0)
    running = jnp.cumsum(log_keep, axis=1)
    block_total = running[:, -1]
    log_w = block_total[:, None, :] - running + log_in
    new_max = jnp.maximum(block_total + stabilizer, lax.optimization_barrier(jnp.max(log_w, axis=1)))
    weights = jnp.exp(log_w - new_max[:, None, :])
    carried = jnp.exp(block_total + stabilizer - new_max)
    weighted_keys = weights[..., None] * key_rows
    cell_new = carried[..., None, None] * cell_state + jnp.einsum('sphd,sphe->shde', weighted_keys, value_rows, precision=highest)
    norm_new = carried[..., None] * normer + lax.optimization_barrier(jnp.sum(weighted_keys, axis=1))
    return (cell_new, norm_new, new_max)

def read_block(queries, key_rows, value_rows, log_in, log_keep, cell_state, normer, stabilizer):
    proposals = queries.shape[1]
    causal = jnp.arange(proposals)[:, None] >= jnp.arange(proposals)[None, :]
    running_h = jnp.moveaxis(jnp.cumsum(log_keep, axis=1), 1, 2)
    input_h = jnp.moveaxis(log_in, 1, 2)
    log_d = jnp.where(causal, running_h[..., :, None] - running_h[..., None, :] + input_h[..., None, :], very_low)
    log_p = running_h + stabilizer[..., None]
    top_log = jnp.maximum(log_p, lax.optimization_barrier(jnp.max(log_d, axis=-1)))
    decays = jnp.exp(log_d - top_log[..., None])
    prior_w = jnp.exp(log_p - top_log)
    scores = jnp.einsum('sthd,suhd->shtu', queries, key_rows, precision=highest) * decays
    numerator = jnp.einsum('shtu,suhe->shte', scores, value_rows, precision=highest)
    numerator = numerator + prior_w[..., None] * jnp.einsum('sthd,shde->shte', queries, cell_state, precision=highest)
    denominator = lax.optimization_barrier(jnp.sum(scores, axis=-1)) + prior_w * jnp.einsum('sthd,shd->sht', queries, normer, precision=highest)
    hidden_out = numerator / jnp.maximum(jnp.abs(denominator), jnp.exp(-top_log))[..., None]
    return jnp.moveaxis(hidden_out, 1, 2)

def reference(tokens, norm_gain, w_query, w_key, w_value, w_outgate, w_gates, forget_bias, head_gain, w_mix, state_cell, state_norm, state_max, pend_keys, pend_values, pend_gates, accepted):
    sequences, proposals, model_width = tokens.shape
    flat_rows = tokens.reshape(sequences * proposals, model_width).astype(jnp.float32)
    row_scale = lax.rsqrt(lax.optimization_barrier(jnp.mean(flat_rows * flat_rows, axis=-1, keepdims=True)) + epsilon)
    scaled_in = (flat_rows * norm_gain).astype(jnp.bfloat16)

    def project(weight):
        return jnp.dot(scaled_in, weight, preferred_element_type=jnp.float32) * row_scale
    queries = project(w_query).astype(jnp.bfloat16)
    new_keys = project(w_key).astype(jnp.bfloat16)
    new_values = project(w_value).astype(jnp.bfloat16)
    outgate = project(w_outgate).astype(jnp.bfloat16)
    gate_pre = project(w_gates.reshape(model_width, 2 * HEADS)).reshape(sequences, proposals, 2, HEADS)

    def split_heads(array):
        return array.astype(jnp.float32).reshape(sequences, proposals, HEADS, HD)
    key_scale = HD ** (-0.5)
    cell_new, norm_new, new_max = fold_pending(state_cell, state_norm, state_max, split_heads(pend_keys) * key_scale, split_heads(pend_values), pend_gates, forget_bias, accepted)
    log_in = gate_pre[:, :, 0, :]
    log_keep = jax.nn.log_sigmoid(gate_pre[:, :, 1, :] + forget_bias)
    hidden = read_block(split_heads(queries), split_heads(new_keys) * key_scale, split_heads(new_values), log_in, log_keep, cell_new, norm_new, new_max)
    normed = hidden * lax.rsqrt(lax.optimization_barrier(jnp.mean(hidden * hidden, axis=-1, keepdims=True)) + epsilon) * head_gain.reshape(HEADS, HD)
    gated_rows = (jax.nn.sigmoid(split_heads(outgate)) * normed).astype(jnp.bfloat16)
    gated_rows = gated_rows.reshape(sequences * proposals, N_TP, BR_W // N_TP)
    group_parts = jnp.einsum('tgc,gcd->gtd', gated_rows.astype(jnp.float32), w_mix.reshape(N_TP, BR_W // N_TP, model_width).astype(jnp.float32)).astype(jnp.bfloat16)
    mixed_out = lax.optimization_barrier(jnp.sum(group_parts.astype(jnp.float32), axis=0)).astype(jnp.bfloat16)
    return (mixed_out.reshape(sequences, proposals, model_width), cell_new, norm_new, new_max)
```

```python
import functools

import jax
import jax.numpy as jnp
from jax import lax
from jax.experimental import pallas as pl
from jax.experimental.pallas import tpu as pltpu
from jax.sharding import PartitionSpec as P

epsilon = 1e-06
very_low = -1e30
highest = lax.Precision.HIGHEST


def shortened(shard):

    def short(part):
        return part.astype(jnp.bfloat16) if part.dtype == jnp.float32 else part

    return jax.tree.map(short, shard)


def from_partner(shard, axis, stride):
    return lax.ppermute(shard, axis, [(i, i ^ 1 << stride) for i in range(lax.axis_size(axis))])


def fold_pending(
    cell_state, normer, stabilizer, key_rows, value_rows, gate_rows, forget_shift, accepted
):
    proposals = key_rows.shape[1]
    accepted_mask = jnp.arange(proposals)[None, :, None] < accepted[:, None, None]
    log_in = jnp.where(accepted_mask, gate_rows[:, :, 0, :], very_low)
    log_keep = jnp.where(
        accepted_mask, jax.nn.log_sigmoid(gate_rows[:, :, 1, :] + forget_shift), 0.0
    )
    running = jnp.cumsum(log_keep, axis=1)
    block_total = running[:, -1]
    log_w = block_total[:, None, :] - running + log_in
    new_max = jnp.maximum(block_total + stabilizer, jnp.max(log_w, axis=1))
    weights = jnp.exp(log_w - new_max[:, None, :])
    carried = jnp.exp(block_total + stabilizer - new_max)
    weighted_keys = weights[..., None] * key_rows
    cell_new = carried[..., None, None] * cell_state + jnp.einsum(
        "sphd,sphe->shde", weighted_keys, value_rows, precision=highest
    )
    norm_new = carried[..., None] * normer + jnp.sum(weighted_keys, axis=1)
    return (cell_new, norm_new, new_max)


def read_block(queries, key_rows, value_rows, log_in, log_keep, cell_state, normer, stabilizer):
    proposals = queries.shape[1]
    causal = jnp.arange(proposals)[:, None] >= jnp.arange(proposals)[None, :]
    running_h = jnp.moveaxis(jnp.cumsum(log_keep, axis=1), 1, 2)
    input_h = jnp.moveaxis(log_in, 1, 2)
    log_d = jnp.where(
        causal, running_h[..., :, None] - running_h[..., None, :] + input_h[..., None, :], very_low
    )
    log_p = running_h + stabilizer[..., None]
    top_log = jnp.maximum(log_p, jnp.max(log_d, axis=-1))
    decays = jnp.exp(log_d - top_log[..., None])
    prior_w = jnp.exp(log_p - top_log)
    scores = jnp.einsum("sthd,suhd->shtu", queries, key_rows, precision=highest) * decays
    numerator = jnp.einsum("shtu,suhe->shte", scores, value_rows, precision=highest)
    numerator = numerator + prior_w[..., None] * jnp.einsum(
        "sthd,shde->shte", queries, cell_state, precision=highest
    )
    denominator = jnp.sum(scores, axis=-1) + prior_w * jnp.einsum(
        "sthd,shd->sht", queries, normer, precision=highest
    )
    hidden_out = numerator / jnp.maximum(jnp.abs(denominator), jnp.exp(-top_log))[..., None]
    return jnp.moveaxis(hidden_out, 1, 2)


def digit_of(own, bit):
    return own // 2**bit % 2


def collect_digits(pieces, dims, own, bits, sender):
    for bit in bits:
        others = sender(pieces, bit)
        first = digit_of(own, bit) == 0
        pieces = tuple(
            (
                jnp.where(
                    first,
                    jnp.concatenate((mine, theirs), axis=dim),
                    jnp.concatenate((theirs, mine), axis=dim),
                )
                for mine, theirs, dim in zip(pieces, others, dims)
            )
        )
    return pieces


def butterfly(blocks, own, near_bits, sender):
    for bit in range(near_bits):
        axis = near_bits - 1 - bit
        mine_digit = digit_of(own, bit)
        kept = lax.dynamic_index_in_dim(blocks, mine_digit, axis, keepdims=False)
        outgoing = lax.dynamic_index_in_dim(blocks, 1 - mine_digit, axis, keepdims=False)
        arrived = sender(outgoing, bit)
        blocks = jnp.where(
            mine_digit == 0,
            jnp.stack((kept, arrived), axis=axis),
            jnp.stack((arrived, kept), axis=axis),
        )
    return blocks


def halving(terms, own, near_bits, sender):
    for bit in range(near_bits - 1, -1, -1):
        mine_digit = digit_of(own, bit)
        kept = tuple(
            (lax.dynamic_index_in_dim(term, mine_digit, 0, keepdims=False) for term in terms)
        )
        outgoing = tuple(
            (lax.dynamic_index_in_dim(term, 1 - mine_digit, 0, keepdims=False) for term in terms)
        )
        arrived = sender(outgoing, bit)
        terms = tuple((left + right for left, right in zip(kept, arrived)))
    return terms


def greet(others):
    barrier = pltpu.get_barrier_semaphore()
    for where in others:
        pl.semaphore_signal(
            barrier, inc=1, device_id=where, device_id_type=pl.DeviceIdType.MESH
        )
    pl.semaphore_wait(barrier, len(others))


def project_kernel(
    ways,
    tok_ref,
    gain_ref,
    wq_ref,
    wk_ref,
    wv_ref,
    wo_ref,
    wg_ref,
    out_ref,
    gate_ref,
    tok_in,
    wg_in,
    part_out,
    part_in,
    total,
    tok_send,
    tok_recv,
    wg_send,
    wg_recv,
    part_send,
    part_recv,
):
    me = lax.axis_index("kv")
    rows = wq_ref.shape[0]
    width = wq_ref.shape[1]
    model_width = tok_ref.shape[1]
    greet([{"kv": lax.rem(me + step, ways)} for step in range(1, ways)])

    def columns(owner):
        return pl.ds(pl.multiple_of(owner * rows, rows), rows)

    sends = []
    for step in range(1, ways):
        there = lax.rem(me + step, ways)
        copy = pltpu.make_async_remote_copy(
            src_ref=tok_ref.at[:, columns(there)],
            dst_ref=tok_in.at[step],
            send_sem=tok_send.at[step],
            recv_sem=tok_recv.at[step],
            device_id={"kv": there},
            device_id_type=pl.DeviceIdType.MESH,
        )
        copy.start()
        sends.append(copy)
    gates_copies = []
    for step in range(1, ways):
        there = lax.rem(me + step, ways)
        copy = pltpu.make_async_remote_copy(
            src_ref=wg_ref,
            dst_ref=wg_in.at[step],
            send_sem=wg_send.at[step],
            recv_sem=wg_recv.at[step],
            device_id={"kv": there},
            device_id_type=pl.DeviceIdType.MESH,
        )
        copy.start()
        gates_copies.append(copy)

    weights = (wq_ref, wk_ref, wv_ref, wo_ref)
    gain = gain_ref[:, columns(me)]

    def scaled(block, gain_part):
        return (block.astype(jnp.float32) * gain_part).astype(jnp.bfloat16)

    part_copies = []
    for step in range(1, ways):
        sends[step - 1].wait_recv()
        block = scaled(tok_in[step], gain)
        for index, weight in enumerate(weights):
            part_out[step, :, index * width : (index + 1) * width] = jnp.dot(
                block, weight[...], preferred_element_type=jnp.float32
            ).astype(jnp.bfloat16)
        back = lax.rem(me - step + ways, ways)
        copy = pltpu.make_async_remote_copy(
            src_ref=part_out.at[step],
            dst_ref=part_in.at[step],
            send_sem=part_send.at[step],
            recv_sem=part_recv.at[step],
            device_id={"kv": back},
            device_id_type=pl.DeviceIdType.MESH,
        )
        copy.start()
        part_copies.append(copy)

    block = scaled(tok_ref[:, columns(me)], gain)
    for index, weight in enumerate(weights):
        total[:, index * width : (index + 1) * width] = jnp.dot(
            block, weight[...], preferred_element_type=jnp.float32
        )
    contract = (((1,), (1,)), ((), ()))
    gates = lax.dot_general(block, wg_ref[...], contract, preferred_element_type=jnp.float32)
    squares = jnp.zeros((tok_ref.shape[0], 1), jnp.float32)
    for step in range(ways):
        part = tok_ref[:, step * rows : (step + 1) * rows].astype(jnp.float32)
        squares = squares + jnp.sum(part * part, axis=1, keepdims=True)
    row_scale = lax.rsqrt(squares / model_width + epsilon)
    for step in range(1, ways):
        gates_copies[step - 1].wait_recv()
        owner = lax.rem(me - step + ways, ways)
        block = scaled(tok_ref[:, columns(owner)], gain_ref[:, columns(owner)])
        gates = gates + lax.dot_general(
            block, wg_in[step], contract, preferred_element_type=jnp.float32
        )
    gate_ref[...] = gates * row_scale

    for step in range(1, ways):
        part_copies[step - 1].wait_recv()
        for index in range(len(weights)):
            place = slice(index * width, (index + 1) * width)
            total[:, place] += part_in[step, :, place].astype(jnp.float32)
    for index in range(len(weights)):
        place = slice(index * width, (index + 1) * width)
        out_ref[:, place] = (total[:, place] * row_scale).astype(jnp.bfloat16)
    for copy in sends + gates_copies + part_copies:
        copy.wait_send()


def project(flat_rows, norm_gain, weights, w_gates):
    ways = lax.axis_size("kv")
    count, model_width = flat_rows.shape
    rows, width = weights[0].shape
    columns = width * len(weights)
    gate_rows = w_gates.shape[1]
    vmem = pl.BlockSpec(memory_space=pltpu.VMEM)
    dma = pltpu.SemaphoreType.DMA((ways,))
    return pl.pallas_call(
        functools.partial(project_kernel, ways),
        out_shape=(
            jax.ShapeDtypeStruct((count, columns), jnp.bfloat16),
            jax.ShapeDtypeStruct((count, gate_rows), jnp.float32),
        ),
        in_specs=[vmem] * 7,
        out_specs=(vmem, vmem),
        scratch_shapes=[
            pltpu.VMEM((ways, count, rows), jnp.bfloat16),
            pltpu.VMEM((ways, gate_rows, rows), jnp.bfloat16),
            pltpu.VMEM((ways, count, columns), jnp.bfloat16),
            pltpu.VMEM((ways, count, columns), jnp.bfloat16),
            pltpu.VMEM((count, columns), jnp.float32),
        ]
        + [dma] * 6,
        compiler_params=pltpu.CompilerParams(collective_id=0, has_side_effects=True),
    )(flat_rows, norm_gain[None, :], *weights, w_gates.T)


def mix_kernel(
    ways,
    groups,
    gated_ref,
    mix_ref,
    out_ref,
    gated_in,
    part_out,
    part_in,
    gated_send,
    gated_recv,
    part_send,
    part_recv,
):
    me = lax.axis_index("kv")
    group = lax.axis_index("tp")
    each = ways // groups
    width = mix_ref.shape[1]
    target = me // each
    spot = lax.rem(me, each) * groups + group
    at_home = target == group
    barrier = pltpu.get_barrier_semaphore()

    def signal(where):
        pl.semaphore_signal(
            barrier, inc=1, device_id=where, device_id_type=pl.DeviceIdType.MESH
        )

    for step in range(1, ways):
        signal({"kv": lax.rem(me + step, ways)})
    for which in range(each):
        for other in range(groups):
            sender = group * each + which

            @pl.when(jnp.logical_or(sender != me, group != other))
            def _():
                signal({"kv": sender, "tp": other})

    @pl.when(at_home)
    def _():
        pl.semaphore_wait(barrier, 2 * (ways - 1))

    @pl.when(jnp.logical_not(at_home))
    def _():
        pl.semaphore_wait(barrier, 2 * (ways - 1) + 1)

    gathers = []
    for step in range(1, ways):
        copy = pltpu.make_async_remote_copy(
            src_ref=gated_ref,
            dst_ref=gated_in.at[step],
            send_sem=gated_send.at[step],
            recv_sem=gated_recv.at[step],
            device_id={"kv": lax.rem(me + step, ways)},
            device_id_type=pl.DeviceIdType.MESH,
        )
        copy.start()
        gathers.append(copy)

    def outgoing(step, owner):
        return pltpu.make_async_remote_copy(
            src_ref=part_out.at[step],
            dst_ref=part_in.at[spot],
            send_sem=part_send.at[step],
            recv_sem=part_recv.at[spot],
            device_id={"kv": owner, "tp": target},
            device_id_type=pl.DeviceIdType.MESH,
        )

    kept = pltpu.make_async_copy(part_out.at[0], part_in.at[spot], part_recv.at[spot])

    def mixed(block):
        return jnp.dot(block, mix_ref[...], preferred_element_type=jnp.float32).astype(
            jnp.bfloat16
        )

    part_out[0] = mixed(gated_ref[...])

    @pl.when(at_home)
    def _():
        kept.start()

    @pl.when(jnp.logical_not(at_home))
    def _():
        outgoing(0, me).start()

    copies = []
    for step in range(1, ways):
        gathers[step - 1].wait_recv()
        part_out[step] = mixed(gated_in[step])
        copy = outgoing(step, lax.rem(me - step + ways, ways))
        copy.start()
        copies.append(copy)

    for which in range(each):
        total = None
        for other in range(groups):
            slot = which * groups + other
            pltpu.make_async_copy(part_out.at[0], part_in.at[slot], part_recv.at[slot]).wait()
            term = part_in[slot].astype(jnp.float32)
            total = term if total is None else total + term
        out_ref[:, which * width : (which + 1) * width] = total.astype(jnp.bfloat16)
    for copy in gathers + copies:
        copy.wait_send()

    @pl.when(jnp.logical_not(at_home))
    def _():
        outgoing(0, me).wait_send()


def mix(gated_rows, w_mix):
    ways, groups = lax.axis_size("kv"), lax.axis_size("tp")
    count, rows = gated_rows.shape
    width = w_mix.shape[1]
    vmem = pl.BlockSpec(memory_space=pltpu.VMEM)
    dma = pltpu.SemaphoreType.DMA((ways,))
    return pl.pallas_call(
        functools.partial(mix_kernel, ways, groups),
        out_shape=jax.ShapeDtypeStruct((count, ways // groups * width), jnp.bfloat16),
        in_specs=[vmem] * 2,
        out_specs=vmem,
        scratch_shapes=[
            pltpu.VMEM((ways, count, rows), jnp.bfloat16),
            pltpu.VMEM((ways, count, width), jnp.bfloat16),
            pltpu.VMEM((ways, count, width), jnp.bfloat16),
        ]
        + [dma] * 4,
        compiler_params=pltpu.CompilerParams(collective_id=1, has_side_effects=True),
    )(gated_rows, w_mix)


def project_by_digits(flat_rows, norm_gain, weights, w_mix):
    token_count, model_width = flat_rows.shape
    shard_rows = weights[0].shape[0]
    own = lax.axis_index("kv")
    kv_bits = lax.axis_size("kv").bit_length() - 1
    near_bits = kv_bits // 2
    near = 2**near_bits
    far = lax.axis_size("kv") // near
    digit_shape = (2,) * near_bits
    collected = collect_digits(
        weights + (w_mix,),
        (0, 0, 0, 0, 0, 1),
        own,
        range(near_bits, kv_bits),
        lambda parts, bit: jax.tree.map(
            lambda part, own: part.astype(own.dtype),
            from_partner(shortened(parts), "kv", bit),
            parts,
        ),
    )
    far_mix = collected[5]
    token_digits = jnp.moveaxis(flat_rows.reshape(token_count, far, near, shard_rows), 2, 0)
    token_digits = token_digits.reshape(digit_shape + (token_count, far, shard_rows))
    arrived = butterfly(
        token_digits, own, near_bits, lambda part, bit: from_partner(part, "kv", bit)
    )
    gathered = arrived.reshape(near * token_count, far * shard_rows)
    gain_part = lax.dynamic_index_in_dim(
        norm_gain.reshape(far, near, shard_rows), own % near, 1, keepdims=False
    ).reshape(far * shard_rows)
    widened = gathered.astype(jnp.float32)
    scaled_in = (widened * gain_part).astype(jnp.bfloat16)
    partials = tuple(
        (
            jnp.dot(scaled_in, weight, preferred_element_type=jnp.float32).reshape(
                digit_shape + (token_count, weight.shape[1])
            )
            for weight in collected[:5]
        )
    )
    part_squares = jnp.sum(widened * widened, axis=-1).reshape(digit_shape + (token_count,))
    summed = halving(
        partials + (part_squares,),
        own,
        near_bits,
        lambda parts, bit: jax.tree.map(
            lambda part, own: part.astype(own.dtype),
            from_partner(shortened(parts), "kv", bit),
            parts,
        ),
    )
    totals = summed[:5]
    sum_squares = summed[5]
    row_scale = lax.rsqrt(sum_squares / model_width + epsilon)[:, None]
    return (
        tuple((total * row_scale).astype(jnp.bfloat16) for total in totals[:4]),
        totals[4] * row_scale,
        far_mix,
    )


def mix_by_digits(gated_rows, far_mix, model_width):
    token_count = gated_rows.shape[0]
    shard_rows = model_width // lax.axis_size("kv")
    own = lax.axis_index("kv")
    kv_bits = lax.axis_size("kv").bit_length() - 1
    near_bits = kv_bits // 2
    near = 2**near_bits
    far = lax.axis_size("kv") // near
    digit_shape = (2,) * near_bits
    near_gated = collect_digits(
        (gated_rows,),
        (0,),
        own,
        range(near_bits),
        lambda parts, bit: jax.tree.map(
            lambda part, own: part.astype(own.dtype),
            from_partner(shortened(parts), "kv", bit),
            parts,
        ),
    )[0]
    group_part = jnp.dot(near_gated, far_mix, preferred_element_type=jnp.float32).astype(
        jnp.bfloat16
    )
    group_part = group_part.reshape(digit_shape + (token_count, far, shard_rows))
    placed = butterfly(group_part, own, near_bits, lambda part, bit: from_partner(part, "kv", bit))
    placed = placed.reshape(near, token_count, far, shard_rows).transpose(1, 2, 0, 3)
    partial_out = placed.reshape(token_count, model_width).astype(jnp.float32)
    mixed_out = lax.psum_scatter(
        partial_out.astype(jnp.bfloat16), "tp", scatter_dimension=1, tiled=True
    )
    return mixed_out


def shards(
    tokens,
    norm_gain,
    w_query,
    w_key,
    w_value,
    w_outgate,
    w_gates,
    forget_bias,
    head_gain,
    w_mix,
    state_cell,
    state_norm,
    state_max,
    pend_keys,
    pend_values,
    pend_gates,
    accepted,
):
    sequences, proposals, model_width = tokens.shape
    token_count = sequences * proposals
    local_heads = forget_bias.shape[0]
    head_size = state_cell.shape[-1]
    shard_rows = w_query.shape[0]
    weights = (w_query, w_key, w_value, w_outgate)
    flat_gates = w_gates.reshape(shard_rows, -1)
    flat_rows = tokens.reshape(token_count, model_width)
    direct = (
        shard_rows % 128 == 0
        and w_mix.shape[1] % 128 == 0
        and lax.axis_size("kv") % lax.axis_size("tp") == 0
    )
    if direct:
        columns, gate_pre = project(flat_rows, norm_gain, weights, flat_gates)
        queries, new_keys, new_values, outgate = jnp.split(columns, len(weights), axis=1)
    else:
        projected, gate_pre, far_mix = project_by_digits(
            flat_rows, norm_gain, weights + (flat_gates,), w_mix
        )
        queries, new_keys, new_values, outgate = projected
    gate_pre = gate_pre.reshape(sequences, proposals, 2, local_heads)

    def split_heads(array):
        return array.astype(jnp.float32).reshape(sequences, proposals, local_heads, head_size)

    key_scale = head_size ** (-0.5)
    cell_new, norm_new, new_max = fold_pending(
        state_cell,
        state_norm,
        state_max,
        split_heads(pend_keys) * key_scale,
        split_heads(pend_values),
        pend_gates,
        forget_bias,
        accepted,
    )
    log_in = gate_pre[:, :, 0, :]
    log_keep = jax.nn.log_sigmoid(gate_pre[:, :, 1, :] + forget_bias)
    hidden = read_block(
        split_heads(queries),
        split_heads(new_keys) * key_scale,
        split_heads(new_values),
        log_in,
        log_keep,
        cell_new,
        norm_new,
        new_max,
    )
    normed = hidden * lax.rsqrt(jnp.mean(hidden * hidden, axis=-1, keepdims=True) + epsilon)
    normed = normed * head_gain.reshape(local_heads, head_size)
    gated_rows = (jax.nn.sigmoid(split_heads(outgate)) * normed).astype(jnp.bfloat16)
    gated_rows = gated_rows.reshape(token_count, local_heads * head_size)
    if direct:
        mixed_out = mix(gated_rows, w_mix)
    else:
        mixed_out = mix_by_digits(gated_rows, far_mix, model_width)
    return (mixed_out.reshape(sequences, proposals, -1), cell_new, norm_new, new_max)


def solution(mesh):
    return jax.shard_map(
        shards,
        mesh=mesh,
        in_specs=(
            P("kv", None, None),
            P(),
            P("kv", "tp"),
            P("kv", "tp"),
            P("kv", "tp"),
            P("kv", "tp"),
            P("kv", None, "tp"),
            P("tp"),
            P("tp"),
            P("tp", "kv"),
            P("kv", "tp", None, None),
            P("kv", "tp", None),
            P("kv", "tp"),
            P("kv", None, "tp"),
            P("kv", None, "tp"),
            P("kv", None, None, "tp"),
            P("kv"),
        ),
        out_specs=(
            P("kv", None, "tp"),
            P("kv", "tp", None, None),
            P("kv", "tp", None),
            P("kv", "tp"),
        ),
        check_vma=False,
    )
```

```python
import functools

import jax
import jax.numpy as jnp
from jax import lax
from jax.experimental import pallas as pl
from jax.experimental.pallas import tpu as pltpu
from jax.sharding import PartitionSpec as P

epsilon = 1e-06
very_low = -1e30
highest = lax.Precision.HIGHEST


def shortened(shard):

    def short(part):
        return part.astype(jnp.bfloat16) if part.dtype == jnp.float32 else part

    return jax.tree.map(short, shard)


def from_partner(shard, axis, stride):
    return lax.ppermute(shard, axis, [(i, i ^ 1 << stride) for i in range(lax.axis_size(axis))])


def running_sum(values):
    steps = values.shape[1]
    upto = jnp.arange(steps)[:, None] >= jnp.arange(steps)[None, :]
    return jnp.sum(jnp.where(upto[None, :, :, None], values[:, None], 0.0), axis=2)


def fold_pending(
    cell_state, normer, stabilizer, key_rows, value_rows, gate_rows, forget_shift, accepted
):
    proposals = key_rows.shape[1]
    accepted_mask = jnp.arange(proposals)[None, :, None] < accepted[:, None, None]
    log_in = jnp.where(accepted_mask, gate_rows[:, :, 0, :], very_low)
    log_keep = jnp.where(
        accepted_mask, jax.nn.log_sigmoid(gate_rows[:, :, 1, :] + forget_shift), 0.0
    )
    running = running_sum(log_keep)
    block_total = running[:, -1]
    log_w = block_total[:, None, :] - running + log_in
    new_max = jnp.maximum(block_total + stabilizer, jnp.max(log_w, axis=1))
    weights = jnp.exp(log_w - new_max[:, None, :])
    carried = jnp.exp(block_total + stabilizer - new_max)
    weighted_keys = weights[..., None] * key_rows
    cell_new = carried[..., None, None] * cell_state + jnp.einsum(
        "sphd,sphe->shde", weighted_keys, value_rows, precision=highest
    )
    norm_new = carried[..., None] * normer + jnp.sum(weighted_keys, axis=1)
    return (cell_new, norm_new, new_max)


def read_block(queries, key_rows, value_rows, log_in, log_keep, cell_state, normer, stabilizer):
    proposals = queries.shape[1]
    causal = jnp.arange(proposals)[:, None] >= jnp.arange(proposals)[None, :]
    running_h = jnp.moveaxis(running_sum(log_keep), 1, 2)
    input_h = jnp.moveaxis(log_in, 1, 2)
    log_d = jnp.where(
        causal, running_h[..., :, None] - running_h[..., None, :] + input_h[..., None, :], very_low
    )
    log_p = running_h + stabilizer[..., None]
    top_log = jnp.maximum(log_p, jnp.max(log_d, axis=-1))
    decays = jnp.exp(log_d - top_log[..., None])
    prior_w = jnp.exp(log_p - top_log)
    scores = jnp.einsum("sthd,suhd->shtu", queries, key_rows, precision=highest) * decays
    numerator = jnp.einsum("shtu,suhe->shte", scores, value_rows, precision=highest)
    numerator = numerator + prior_w[..., None] * jnp.einsum(
        "sthd,shde->shte", queries, cell_state, precision=highest
    )
    denominator = jnp.sum(scores, axis=-1) + prior_w * jnp.einsum(
        "sthd,shd->sht", queries, normer, precision=highest
    )
    hidden_out = numerator / jnp.maximum(jnp.abs(denominator), jnp.exp(-top_log))[..., None]
    return jnp.moveaxis(hidden_out, 1, 2)


def digit_of(own, bit):
    return own // 2**bit % 2


def collect_digits(pieces, dims, own, bits, sender):
    for bit in bits:
        others = sender(pieces, bit)
        first = digit_of(own, bit) == 0
        pieces = tuple(
            (
                jnp.where(
                    first,
                    jnp.concatenate((mine, theirs), axis=dim),
                    jnp.concatenate((theirs, mine), axis=dim),
                )
                for mine, theirs, dim in zip(pieces, others, dims)
            )
        )
    return pieces


def butterfly(blocks, own, near_bits, sender):
    for bit in range(near_bits):
        axis = near_bits - 1 - bit
        mine_digit = digit_of(own, bit)
        kept = lax.dynamic_index_in_dim(blocks, mine_digit, axis, keepdims=False)
        outgoing = lax.dynamic_index_in_dim(blocks, 1 - mine_digit, axis, keepdims=False)
        arrived = sender(outgoing, bit)
        blocks = jnp.where(
            mine_digit == 0,
            jnp.stack((kept, arrived), axis=axis),
            jnp.stack((arrived, kept), axis=axis),
        )
    return blocks


def halving(terms, own, near_bits, sender):
    for bit in range(near_bits - 1, -1, -1):
        mine_digit = digit_of(own, bit)
        kept = tuple(
            (lax.dynamic_index_in_dim(term, mine_digit, 0, keepdims=False) for term in terms)
        )
        outgoing = tuple(
            (lax.dynamic_index_in_dim(term, 1 - mine_digit, 0, keepdims=False) for term in terms)
        )
        arrived = sender(outgoing, bit)
        terms = tuple((left + right for left, right in zip(kept, arrived)))
    return terms


def greet(others):
    barrier = pltpu.get_barrier_semaphore()
    for where in others:
        pl.semaphore_signal(
            barrier, inc=1, device_id=where, device_id_type=pl.DeviceIdType.MESH
        )
    pl.semaphore_wait(barrier, len(others))


def project_kernel(
    ways,
    tok_ref,
    gain_ref,
    wq_ref,
    wk_ref,
    wv_ref,
    wo_ref,
    wg_ref,
    out_ref,
    gate_ref,
    tok_in,
    wg_in,
    pair_out,
    pair_in,
    far_out,
    far_in,
    total,
    tok_send,
    tok_recv,
    wg_send,
    wg_recv,
    pair_send,
    pair_recv,
    far_send,
    far_recv,
):
    me = lax.axis_index("kv")
    far = ways // 2
    place, side = me // 2, lax.rem(me, 2)
    rows = wq_ref.shape[0]
    width = wq_ref.shape[1]
    model_width = tok_ref.shape[1]

    def ahead(hop, other):
        return 2 * lax.rem(place + hop, far) + (1 - side if other else side)

    def behind(hop, other):
        return 2 * lax.rem(place - hop + far, far) + (1 - side if other else side)

    def columns(owner):
        return pl.ds(pl.multiple_of(owner * rows, rows), rows)

    def remote(source, target, send_sem, recv_sem, there):
        copy = pltpu.make_async_remote_copy(
            src_ref=source,
            dst_ref=target,
            send_sem=send_sem,
            recv_sem=recv_sem,
            device_id={"kv": there},
            device_id_type=pl.DeviceIdType.MESH,
        )
        copy.start()
        return copy

    hops = list(range(1, far))
    peers = [(0, 1)] + [(hop, 1) for hop in hops] + [(hop, 0) for hop in hops]
    greet([{"kv": ahead(hop, other)} for hop, other in peers])

    tok_copies, wg_copies = {}, {}
    for hop, other in peers:
        slot = 2 * hop + other
        there = ahead(hop, other)
        tok_copies[slot] = remote(
            tok_ref.at[:, columns(there)],
            tok_in.at[slot],
            tok_send.at[slot],
            tok_recv.at[slot],
            there,
        )
    for hop, other in peers:
        slot = 2 * hop + other
        wg_copies[slot] = remote(
            wg_ref, wg_in.at[slot], wg_send.at[slot], wg_recv.at[slot], ahead(hop, other)
        )

    weights = (wq_ref, wk_ref, wv_ref, wo_ref)
    spans = [slice(index * width, (index + 1) * width) for index in range(len(weights))]
    gain = gain_ref[:, columns(me)]

    def scaled(block, gain_part):
        return (block.astype(jnp.float32) * gain_part).astype(jnp.bfloat16)

    def times(block, weight):
        return jnp.dot(block, weight[...], preferred_element_type=jnp.float32)

    pair_copies, far_copies = [], []
    for hop in [0] + hops:
        slot = 2 * hop + 1
        tok_copies[slot].wait_recv()
        block = scaled(tok_in[slot], gain)
        for span, weight in zip(spans, weights):
            pair_out[hop, :, span] = times(block, weight).astype(jnp.bfloat16)
        pair_copies.append(
            remote(
                pair_out.at[hop],
                pair_in.at[hop],
                pair_send.at[hop],
                pair_recv.at[hop],
                behind(0, 1),
            )
        )

    own_block = scaled(tok_ref[:, columns(me)], gain)
    for span, weight in zip(spans, weights):
        total[:, span] = times(own_block, weight)
    squares = jnp.zeros((tok_ref.shape[0], 1), jnp.float32)
    for step in range(ways):
        part = tok_ref[:, step * rows : (step + 1) * rows].astype(jnp.float32)
        squares = squares + jnp.sum(part * part, axis=1, keepdims=True)
    row_scale = lax.rsqrt(squares / model_width + epsilon)

    for hop in hops:
        slot = 2 * hop
        tok_copies[slot].wait_recv()
        block = scaled(tok_in[slot], gain)
        pair_copies[hop].wait_recv()
        for span, weight in zip(spans, weights):
            far_out[hop, :, span] = (
                times(block, weight) + pair_in[hop, :, span].astype(jnp.float32)
            ).astype(jnp.bfloat16)
        far_copies.append(
            remote(
                far_out.at[hop],
                far_in.at[hop],
                far_send.at[hop],
                far_recv.at[hop],
                behind(hop, 0),
            )
        )

    contract = (((1,), (1,)), ((), ()))
    gates = lax.dot_general(own_block, wg_ref[...], contract, preferred_element_type=jnp.float32)
    for hop, other in peers:
        slot = 2 * hop + other
        wg_copies[slot].wait_recv()
        owner = behind(hop, other)
        block = scaled(tok_ref[:, columns(owner)], gain_ref[:, columns(owner)])
        gates = gates + lax.dot_general(
            block, wg_in[slot], contract, preferred_element_type=jnp.float32
        )
    gate_ref[...] = gates * row_scale

    pair_copies[0].wait_recv()
    for span in spans:
        total[:, span] += pair_in[0, :, span].astype(jnp.float32)
    for hop in hops:
        far_copies[hop - 1].wait_recv()
        for span in spans:
            total[:, span] += far_in[hop, :, span].astype(jnp.float32)
    for span in spans:
        out_ref[:, span] = (total[:, span] * row_scale).astype(jnp.bfloat16)
    for copy in list(tok_copies.values()) + list(wg_copies.values()) + pair_copies + far_copies:
        copy.wait_send()


def project(flat_rows, norm_gain, weights, w_gates):
    ways = lax.axis_size("kv")
    far = ways // 2
    count, model_width = flat_rows.shape
    rows, width = weights[0].shape
    columns = width * len(weights)
    gate_rows = w_gates.shape[1]
    vmem = pl.BlockSpec(memory_space=pltpu.VMEM)
    return pl.pallas_call(
        functools.partial(project_kernel, ways),
        out_shape=(
            jax.ShapeDtypeStruct((count, columns), jnp.bfloat16),
            jax.ShapeDtypeStruct((count, gate_rows), jnp.float32),
        ),
        in_specs=[vmem] * 7,
        out_specs=(vmem, vmem),
        scratch_shapes=[
            pltpu.VMEM((ways, count, rows), jnp.bfloat16),
            pltpu.VMEM((ways, gate_rows, rows), jnp.bfloat16),
        ]
        + [pltpu.VMEM((far, count, columns), jnp.bfloat16)] * 4
        + [pltpu.VMEM((count, columns), jnp.float32)]
        + [pltpu.SemaphoreType.DMA((ways,))] * 4
        + [pltpu.SemaphoreType.DMA((far,))] * 4,
        compiler_params=pltpu.CompilerParams(collective_id=0, has_side_effects=True),
    )(flat_rows, norm_gain[None, :], *weights, w_gates.T)


def mix_kernel(
    ways,
    groups,
    gated_ref,
    mix_ref,
    out_ref,
    gated_in,
    part_out,
    part_in,
    gated_send,
    gated_recv,
    part_send,
    part_recv,
):
    me = lax.axis_index("kv")
    group = lax.axis_index("tp")
    each = ways // groups
    width = mix_ref.shape[1]
    target = me // each
    spot = lax.rem(me, each) * groups + group
    at_home = target == group
    barrier = pltpu.get_barrier_semaphore()

    def signal(where):
        pl.semaphore_signal(
            barrier, inc=1, device_id=where, device_id_type=pl.DeviceIdType.MESH
        )

    for step in range(1, ways):
        signal({"kv": lax.rem(me + step, ways)})
    for which in range(each):
        for other in range(groups):
            sender = group * each + which

            @pl.when(jnp.logical_or(sender != me, group != other))
            def _():
                signal({"kv": sender, "tp": other})

    @pl.when(at_home)
    def _():
        pl.semaphore_wait(barrier, 2 * (ways - 1))

    @pl.when(jnp.logical_not(at_home))
    def _():
        pl.semaphore_wait(barrier, 2 * (ways - 1) + 1)

    gathers = []
    for step in range(1, ways):
        copy = pltpu.make_async_remote_copy(
            src_ref=gated_ref,
            dst_ref=gated_in.at[step],
            send_sem=gated_send.at[step],
            recv_sem=gated_recv.at[step],
            device_id={"kv": lax.rem(me + step, ways)},
            device_id_type=pl.DeviceIdType.MESH,
        )
        copy.start()
        gathers.append(copy)

    def outgoing(step, owner):
        return pltpu.make_async_remote_copy(
            src_ref=part_out.at[step],
            dst_ref=part_in.at[spot],
            send_sem=part_send.at[step],
            recv_sem=part_recv.at[spot],
            device_id={"kv": owner, "tp": target},
            device_id_type=pl.DeviceIdType.MESH,
        )

    kept = pltpu.make_async_copy(part_out.at[0], part_in.at[spot], part_recv.at[spot])

    def mixed(block):
        return jnp.dot(block, mix_ref[...], preferred_element_type=jnp.float32).astype(
            jnp.bfloat16
        )

    part_out[0] = mixed(gated_ref[...])

    @pl.when(at_home)
    def _():
        kept.start()

    @pl.when(jnp.logical_not(at_home))
    def _():
        outgoing(0, me).start()

    copies = []
    for step in range(1, ways):
        gathers[step - 1].wait_recv()
        part_out[step] = mixed(gated_in[step])
        copy = outgoing(step, lax.rem(me - step + ways, ways))
        copy.start()
        copies.append(copy)

    for which in range(each):
        total = None
        for other in range(groups):
            slot = which * groups + other
            pltpu.make_async_copy(part_out.at[0], part_in.at[slot], part_recv.at[slot]).wait()
            term = part_in[slot].astype(jnp.float32)
            total = term if total is None else total + term
        out_ref[:, which * width : (which + 1) * width] = total.astype(jnp.bfloat16)
    for copy in gathers + copies:
        copy.wait_send()

    @pl.when(jnp.logical_not(at_home))
    def _():
        outgoing(0, me).wait_send()


def mix(gated_rows, w_mix):
    ways, groups = lax.axis_size("kv"), lax.axis_size("tp")
    count, rows = gated_rows.shape
    width = w_mix.shape[1]
    vmem = pl.BlockSpec(memory_space=pltpu.VMEM)
    dma = pltpu.SemaphoreType.DMA((ways,))
    return pl.pallas_call(
        functools.partial(mix_kernel, ways, groups),
        out_shape=jax.ShapeDtypeStruct((count, ways // groups * width), jnp.bfloat16),
        in_specs=[vmem] * 2,
        out_specs=vmem,
        scratch_shapes=[
            pltpu.VMEM((ways, count, rows), jnp.bfloat16),
            pltpu.VMEM((ways, count, width), jnp.bfloat16),
            pltpu.VMEM((ways, count, width), jnp.bfloat16),
        ]
        + [dma] * 4,
        compiler_params=pltpu.CompilerParams(collective_id=1, has_side_effects=True),
    )(gated_rows, w_mix)


def project_by_digits(flat_rows, norm_gain, weights, w_mix):
    token_count, model_width = flat_rows.shape
    shard_rows = weights[0].shape[0]
    own = lax.axis_index("kv")
    kv_bits = lax.axis_size("kv").bit_length() - 1
    near_bits = kv_bits // 2
    near = 2**near_bits
    far = lax.axis_size("kv") // near
    digit_shape = (2,) * near_bits
    collected = collect_digits(
        weights + (w_mix,),
        (0, 0, 0, 0, 0, 1),
        own,
        range(near_bits, kv_bits),
        lambda parts, bit: jax.tree.map(
            lambda part, own: part.astype(own.dtype),
            from_partner(shortened(parts), "kv", bit),
            parts,
        ),
    )
    far_mix = collected[5]
    token_digits = jnp.moveaxis(flat_rows.reshape(token_count, far, near, shard_rows), 2, 0)
    token_digits = token_digits.reshape(digit_shape + (token_count, far, shard_rows))
    arrived = butterfly(
        token_digits, own, near_bits, lambda part, bit: from_partner(part, "kv", bit)
    )
    gathered = arrived.reshape(near * token_count, far * shard_rows)
    gain_part = lax.dynamic_index_in_dim(
        norm_gain.reshape(far, near, shard_rows), own % near, 1, keepdims=False
    ).reshape(far * shard_rows)
    widened = gathered.astype(jnp.float32)
    scaled_in = (widened * gain_part).astype(jnp.bfloat16)
    partials = tuple(
        (
            jnp.dot(scaled_in, weight, preferred_element_type=jnp.float32).reshape(
                digit_shape + (token_count, weight.shape[1])
            )
            for weight in collected[:5]
        )
    )
    part_squares = jnp.sum(widened * widened, axis=-1).reshape(digit_shape + (token_count,))
    summed = halving(
        partials + (part_squares,),
        own,
        near_bits,
        lambda parts, bit: jax.tree.map(
            lambda part, own: part.astype(own.dtype),
            from_partner(shortened(parts), "kv", bit),
            parts,
        ),
    )
    totals = summed[:5]
    sum_squares = summed[5]
    row_scale = lax.rsqrt(sum_squares / model_width + epsilon)[:, None]
    return (
        tuple((total * row_scale).astype(jnp.bfloat16) for total in totals[:4]),
        totals[4] * row_scale,
        far_mix,
    )


def mix_by_digits(gated_rows, far_mix, model_width):
    token_count = gated_rows.shape[0]
    shard_rows = model_width // lax.axis_size("kv")
    own = lax.axis_index("kv")
    kv_bits = lax.axis_size("kv").bit_length() - 1
    near_bits = kv_bits // 2
    near = 2**near_bits
    far = lax.axis_size("kv") // near
    digit_shape = (2,) * near_bits
    near_gated = collect_digits(
        (gated_rows,),
        (0,),
        own,
        range(near_bits),
        lambda parts, bit: jax.tree.map(
            lambda part, own: part.astype(own.dtype),
            from_partner(shortened(parts), "kv", bit),
            parts,
        ),
    )[0]
    group_part = jnp.dot(near_gated, far_mix, preferred_element_type=jnp.float32).astype(
        jnp.bfloat16
    )
    group_part = group_part.reshape(digit_shape + (token_count, far, shard_rows))
    placed = butterfly(group_part, own, near_bits, lambda part, bit: from_partner(part, "kv", bit))
    placed = placed.reshape(near, token_count, far, shard_rows).transpose(1, 2, 0, 3)
    partial_out = placed.reshape(token_count, model_width).astype(jnp.float32)
    mixed_out = lax.psum_scatter(
        partial_out.astype(jnp.bfloat16), "tp", scatter_dimension=1, tiled=True
    )
    return mixed_out


def shards(
    tokens,
    norm_gain,
    w_query,
    w_key,
    w_value,
    w_outgate,
    w_gates,
    forget_bias,
    head_gain,
    w_mix,
    state_cell,
    state_norm,
    state_max,
    pend_keys,
    pend_values,
    pend_gates,
    accepted,
):
    sequences, proposals, model_width = tokens.shape
    token_count = sequences * proposals
    local_heads = forget_bias.shape[0]
    head_size = state_cell.shape[-1]
    shard_rows = w_query.shape[0]
    weights = (w_query, w_key, w_value, w_outgate)
    flat_gates = w_gates.reshape(shard_rows, -1)
    flat_rows = tokens.reshape(token_count, model_width)
    direct = (
        shard_rows % 128 == 0
        and w_mix.shape[1] % 128 == 0
        and lax.axis_size("kv") % 2 == 0
        and lax.axis_size("kv") % lax.axis_size("tp") == 0
    )
    if direct:
        columns, gate_pre = project(flat_rows, norm_gain, weights, flat_gates)
        queries, new_keys, new_values, outgate = jnp.split(columns, len(weights), axis=1)
    else:
        projected, gate_pre, far_mix = project_by_digits(
            flat_rows, norm_gain, weights + (flat_gates,), w_mix
        )
        queries, new_keys, new_values, outgate = projected
    gate_pre = gate_pre.reshape(sequences, proposals, 2, local_heads)

    def split_heads(array):
        return array.astype(jnp.float32).reshape(sequences, proposals, local_heads, head_size)

    key_scale = head_size ** (-0.5)
    cell_new, norm_new, new_max = fold_pending(
        state_cell,
        state_norm,
        state_max,
        split_heads(pend_keys) * key_scale,
        split_heads(pend_values),
        pend_gates,
        forget_bias,
        accepted,
    )
    log_in = gate_pre[:, :, 0, :]
    log_keep = jax.nn.log_sigmoid(gate_pre[:, :, 1, :] + forget_bias)
    hidden = read_block(
        split_heads(queries),
        split_heads(new_keys) * key_scale,
        split_heads(new_values),
        log_in,
        log_keep,
        cell_new,
        norm_new,
        new_max,
    )
    normed = hidden * lax.rsqrt(jnp.mean(hidden * hidden, axis=-1, keepdims=True) + epsilon)
    normed = normed * head_gain.reshape(local_heads, head_size)
    gated_rows = (jax.nn.sigmoid(split_heads(outgate)) * normed).astype(jnp.bfloat16)
    gated_rows = gated_rows.reshape(token_count, local_heads * head_size)
    if direct:
        mixed_out = mix(gated_rows, w_mix)
    else:
        mixed_out = mix_by_digits(gated_rows, far_mix, model_width)
    return (mixed_out.reshape(sequences, proposals, -1), cell_new, norm_new, new_max)


def solution(mesh):
    return jax.shard_map(
        shards,
        mesh=mesh,
        in_specs=(
            P("kv", None, None),
            P(),
            P("kv", "tp"),
            P("kv", "tp"),
            P("kv", "tp"),
            P("kv", "tp"),
            P("kv", None, "tp"),
            P("tp"),
            P("tp"),
            P("tp", "kv"),
            P("kv", "tp", None, None),
            P("kv", "tp", None),
            P("kv", "tp"),
            P("kv", None, "tp"),
            P("kv", None, "tp"),
            P("kv", None, None, "tp"),
            P("kv"),
        ),
        out_specs=(
            P("kv", None, "tp"),
            P("kv", "tp", None, None),
            P("kv", "tp", None),
            P("kv", "tp"),
        ),
        check_vma=False,
    )
```

```python
import functools

import jax
import jax.numpy as jnp
from jax import lax
from jax.experimental import pallas as pl
from jax.experimental.pallas import tpu as pltpu
from jax.sharding import PartitionSpec as P

epsilon = 1e-06
very_low = -1e30
highest = lax.Precision.HIGHEST


def shortened(shard):

    def short(part):
        return part.astype(jnp.bfloat16) if part.dtype == jnp.float32 else part

    return jax.tree.map(short, shard)


def from_partner(shard, axis, stride):
    return lax.ppermute(shard, axis, [(i, i ^ 1 << stride) for i in range(lax.axis_size(axis))])


def running_sum(values):
    steps = values.shape[1]
    upto = jnp.arange(steps)[:, None] >= jnp.arange(steps)[None, :]
    return jnp.sum(jnp.where(upto[None, :, :, None], values[:, None], 0.0), axis=2)


def fold_pending(
    cell_state, normer, stabilizer, key_rows, value_rows, gate_rows, forget_shift, accepted
):
    proposals = key_rows.shape[1]
    accepted_mask = jnp.arange(proposals)[None, :, None] < accepted[:, None, None]
    log_in = jnp.where(accepted_mask, gate_rows[:, :, 0, :], very_low)
    log_keep = jnp.where(
        accepted_mask, jax.nn.log_sigmoid(gate_rows[:, :, 1, :] + forget_shift), 0.0
    )
    running = running_sum(log_keep)
    block_total = running[:, -1]
    log_w = block_total[:, None, :] - running + log_in
    new_max = jnp.maximum(block_total + stabilizer, jnp.max(log_w, axis=1))
    weights = jnp.exp(log_w - new_max[:, None, :])
    carried = jnp.exp(block_total + stabilizer - new_max)
    weighted_keys = weights[..., None] * key_rows
    cell_new = carried[..., None, None] * cell_state + jnp.einsum(
        "sphd,sphe->shde", weighted_keys, value_rows, precision=highest
    )
    norm_new = carried[..., None] * normer + jnp.sum(weighted_keys, axis=1)
    return (cell_new, norm_new, new_max)


def read_block(queries, key_rows, value_rows, log_in, log_keep, cell_state, normer, stabilizer):
    proposals = queries.shape[1]
    causal = jnp.arange(proposals)[:, None] >= jnp.arange(proposals)[None, :]
    running_h = jnp.moveaxis(running_sum(log_keep), 1, 2)
    input_h = jnp.moveaxis(log_in, 1, 2)
    log_d = jnp.where(
        causal, running_h[..., :, None] - running_h[..., None, :] + input_h[..., None, :], very_low
    )
    log_p = running_h + stabilizer[..., None]
    top_log = jnp.maximum(log_p, jnp.max(log_d, axis=-1))
    decays = jnp.exp(log_d - top_log[..., None])
    prior_w = jnp.exp(log_p - top_log)
    scores = jnp.einsum("sthd,suhd->shtu", queries, key_rows, precision=highest) * decays
    numerator = jnp.einsum("shtu,suhe->shte", scores, value_rows, precision=highest)
    numerator = numerator + prior_w[..., None] * jnp.einsum(
        "sthd,shde->shte", queries, cell_state, precision=highest
    )
    denominator = jnp.sum(scores, axis=-1) + prior_w * jnp.einsum(
        "sthd,shd->sht", queries, normer, precision=highest
    )
    hidden_out = numerator / jnp.maximum(jnp.abs(denominator), jnp.exp(-top_log))[..., None]
    return jnp.moveaxis(hidden_out, 1, 2)


def digit_of(own, bit):
    return own // 2**bit % 2


def collect_digits(pieces, dims, own, bits, sender):
    for bit in bits:
        others = sender(pieces, bit)
        first = digit_of(own, bit) == 0
        pieces = tuple(
            (
                jnp.where(
                    first,
                    jnp.concatenate((mine, theirs), axis=dim),
                    jnp.concatenate((theirs, mine), axis=dim),
                )
                for mine, theirs, dim in zip(pieces, others, dims)
            )
        )
    return pieces


def butterfly(blocks, own, near_bits, sender):
    for bit in range(near_bits):
        axis = near_bits - 1 - bit
        mine_digit = digit_of(own, bit)
        kept = lax.dynamic_index_in_dim(blocks, mine_digit, axis, keepdims=False)
        outgoing = lax.dynamic_index_in_dim(blocks, 1 - mine_digit, axis, keepdims=False)
        arrived = sender(outgoing, bit)
        blocks = jnp.where(
            mine_digit == 0,
            jnp.stack((kept, arrived), axis=axis),
            jnp.stack((arrived, kept), axis=axis),
        )
    return blocks


def halving(terms, own, near_bits, sender):
    for bit in range(near_bits - 1, -1, -1):
        mine_digit = digit_of(own, bit)
        kept = tuple(
            (lax.dynamic_index_in_dim(term, mine_digit, 0, keepdims=False) for term in terms)
        )
        outgoing = tuple(
            (lax.dynamic_index_in_dim(term, 1 - mine_digit, 0, keepdims=False) for term in terms)
        )
        arrived = sender(outgoing, bit)
        terms = tuple((left + right for left, right in zip(kept, arrived)))
    return terms


def greet(others):
    barrier = pltpu.get_barrier_semaphore()
    for where in others:
        pl.semaphore_signal(
            barrier, inc=1, device_id=where, device_id_type=pl.DeviceIdType.MESH
        )
    pl.semaphore_wait(barrier, len(others))


def project_kernel(
    ways,
    tok_ref,
    gain_ref,
    wq_ref,
    wk_ref,
    wv_ref,
    wo_ref,
    wg_ref,
    out_ref,
    gate_ref,
    tok_in,
    wg_in,
    pair_out,
    pair_in,
    far_out,
    far_in,
    total,
    tok_send,
    tok_recv,
    wg_send,
    wg_recv,
    pair_send,
    pair_recv,
    far_send,
    far_recv,
):
    me = lax.axis_index("kv")
    far = ways // 2
    place, side = me // 2, lax.rem(me, 2)
    rows = wq_ref.shape[0]
    width = wq_ref.shape[1]
    model_width = tok_ref.shape[1]

    def ahead(hop, other):
        return 2 * lax.rem(place + hop, far) + (1 - side if other else side)

    def behind(hop, other):
        return 2 * lax.rem(place - hop + far, far) + (1 - side if other else side)

    def columns(owner):
        return pl.ds(pl.multiple_of(owner * rows, rows), rows)

    def remote(source, target, send_sem, recv_sem, there):
        copy = pltpu.make_async_remote_copy(
            src_ref=source,
            dst_ref=target,
            send_sem=send_sem,
            recv_sem=recv_sem,
            device_id={"kv": there},
            device_id_type=pl.DeviceIdType.MESH,
        )
        copy.start()
        return copy

    hops = list(range(1, far))
    peers = [(hop, 1) for hop in hops] + [(0, 1)] + [(hop, 0) for hop in hops]
    greet([{"kv": ahead(hop, other)} for hop, other in peers])

    tok_copies, wg_copies = {}, {}
    for hop, other in peers:
        slot = 2 * hop + other
        there = ahead(hop, other)
        tok_copies[slot] = remote(
            tok_ref.at[:, columns(there)],
            tok_in.at[slot],
            tok_send.at[slot],
            tok_recv.at[slot],
            there,
        )
    for hop, other in peers:
        slot = 2 * hop + other
        wg_copies[slot] = remote(
            wg_ref, wg_in.at[slot], wg_send.at[slot], wg_recv.at[slot], ahead(hop, other)
        )

    weights = (wq_ref, wk_ref, wv_ref, wo_ref)
    spans = [slice(index * width, (index + 1) * width) for index in range(len(weights))]
    gain = gain_ref[:, columns(me)]

    def scaled(block, gain_part):
        return (block.astype(jnp.float32) * gain_part).astype(jnp.bfloat16)

    def times(block, weight):
        return jnp.dot(block, weight[...], preferred_element_type=jnp.float32)

    halves = (slice(0, 2 * width), slice(2 * width, 4 * width))
    pair_copies, far_copies = {}, {}
    for hop in hops + [0]:
        slot = 2 * hop + 1
        tok_copies[slot].wait_recv()
        block = scaled(tok_in[slot], gain)
        for half, cut in enumerate(halves):
            for index in (2 * half, 2 * half + 1):
                pair_out[hop, :, spans[index]] = times(block, weights[index]).astype(jnp.bfloat16)
            pair_copies[hop, half] = remote(
                pair_out.at[hop, :, cut],
                pair_in.at[hop, :, cut],
                pair_send.at[2 * hop + half],
                pair_recv.at[2 * hop + half],
                behind(0, 1),
            )

    own_block = scaled(tok_ref[:, columns(me)], gain)
    for span, weight in zip(spans, weights):
        total[:, span] = times(own_block, weight)
    squares = jnp.zeros((tok_ref.shape[0], 1), jnp.float32)
    for step in range(ways):
        part = tok_ref[:, step * rows : (step + 1) * rows].astype(jnp.float32)
        squares = squares + jnp.sum(part * part, axis=1, keepdims=True)
    row_scale = lax.rsqrt(squares / model_width + epsilon)

    for hop in hops:
        slot = 2 * hop
        tok_copies[slot].wait_recv()
        block = scaled(tok_in[slot], gain)
        for half, cut in enumerate(halves):
            pair_copies[hop, half].wait_recv()
            for index in (2 * half, 2 * half + 1):
                span = spans[index]
                far_out[hop, :, span] = (
                    times(block, weights[index]) + pair_in[hop, :, span].astype(jnp.float32)
                ).astype(jnp.bfloat16)
            far_copies[hop, half] = remote(
                far_out.at[hop, :, cut],
                far_in.at[hop, :, cut],
                far_send.at[2 * hop + half],
                far_recv.at[2 * hop + half],
                behind(hop, 0),
            )

    contract = (((1,), (1,)), ((), ()))
    gates = lax.dot_general(own_block, wg_ref[...], contract, preferred_element_type=jnp.float32)
    for hop, other in peers:
        slot = 2 * hop + other
        wg_copies[slot].wait_recv()
        owner = behind(hop, other)
        block = scaled(tok_ref[:, columns(owner)], gain_ref[:, columns(owner)])
        gates = gates + lax.dot_general(
            block, wg_in[slot], contract, preferred_element_type=jnp.float32
        )
    gate_ref[...] = gates * row_scale

    pair_copies[0, 0].wait_recv()
    pair_copies[0, 1].wait_recv()
    for span in spans:
        total[:, span] += pair_in[0, :, span].astype(jnp.float32)
    for hop in hops:
        far_copies[hop, 0].wait_recv()
        far_copies[hop, 1].wait_recv()
        for span in spans:
            total[:, span] += far_in[hop, :, span].astype(jnp.float32)
    for span in spans:
        out_ref[:, span] = (total[:, span] * row_scale).astype(jnp.bfloat16)
    for group in (tok_copies, wg_copies, pair_copies, far_copies):
        for copy in group.values():
            copy.wait_send()


def project(flat_rows, norm_gain, weights, w_gates):
    ways = lax.axis_size("kv")
    far = ways // 2
    count, model_width = flat_rows.shape
    rows, width = weights[0].shape
    columns = width * len(weights)
    gate_rows = w_gates.shape[1]
    vmem = pl.BlockSpec(memory_space=pltpu.VMEM)
    return pl.pallas_call(
        functools.partial(project_kernel, ways),
        out_shape=(
            jax.ShapeDtypeStruct((count, columns), jnp.bfloat16),
            jax.ShapeDtypeStruct((count, gate_rows), jnp.float32),
        ),
        in_specs=[vmem] * 7,
        out_specs=(vmem, vmem),
        scratch_shapes=[
            pltpu.VMEM((ways, count, rows), jnp.bfloat16),
            pltpu.VMEM((ways, gate_rows, rows), jnp.bfloat16),
        ]
        + [pltpu.VMEM((far, count, columns), jnp.bfloat16)] * 4
        + [pltpu.VMEM((count, columns), jnp.float32)]
        + [pltpu.SemaphoreType.DMA((ways,))] * 8,
        compiler_params=pltpu.CompilerParams(collective_id=0, has_side_effects=True),
    )(flat_rows, norm_gain[None, :], *weights, w_gates.T)


def mix_kernel(
    ways,
    groups,
    gated_ref,
    mix_ref,
    out_ref,
    gated_in,
    part_out,
    part_in,
    gated_send,
    gated_recv,
    part_send,
    part_recv,
):
    me = lax.axis_index("kv")
    group = lax.axis_index("tp")
    each = ways // groups
    width = mix_ref.shape[1]
    target = me // each
    spot = lax.rem(me, each) * groups + group
    at_home = target == group
    barrier = pltpu.get_barrier_semaphore()

    def signal(where):
        pl.semaphore_signal(
            barrier, inc=1, device_id=where, device_id_type=pl.DeviceIdType.MESH
        )

    for step in range(1, ways):
        signal({"kv": lax.rem(me + step, ways)})
    for which in range(each):
        for other in range(groups):
            sender = group * each + which

            @pl.when(jnp.logical_or(sender != me, group != other))
            def _():
                signal({"kv": sender, "tp": other})

    @pl.when(at_home)
    def _():
        pl.semaphore_wait(barrier, 2 * (ways - 1))

    @pl.when(jnp.logical_not(at_home))
    def _():
        pl.semaphore_wait(barrier, 2 * (ways - 1) + 1)

    far = ways // 2
    place, side = me // 2, lax.rem(me, 2)
    partner = 2 * place + 1 - side
    hops = list(range(1, far))

    def gather(source, slot, there):
        copy = pltpu.make_async_remote_copy(
            src_ref=source,
            dst_ref=gated_in.at[slot],
            send_sem=gated_send.at[slot],
            recv_sem=gated_recv.at[slot],
            device_id={"kv": there},
            device_id_type=pl.DeviceIdType.MESH,
        )
        copy.start()
        return copy

    gathers = {}
    for hop in hops:
        gathers[2 * hop] = gather(gated_ref, 2 * hop, 2 * lax.rem(place + hop, far) + side)
    gathers[1] = gather(gated_ref, 1, partner)

    def outgoing(step, owner):
        return pltpu.make_async_remote_copy(
            src_ref=part_out.at[step],
            dst_ref=part_in.at[spot],
            send_sem=part_send.at[step],
            recv_sem=part_recv.at[spot],
            device_id={"kv": owner, "tp": target},
            device_id_type=pl.DeviceIdType.MESH,
        )

    kept = pltpu.make_async_copy(part_out.at[0], part_in.at[spot], part_recv.at[spot])

    def mixed(block):
        return jnp.dot(block, mix_ref[...], preferred_element_type=jnp.float32).astype(
            jnp.bfloat16
        )

    part_out[0] = mixed(gated_ref[...])

    @pl.when(at_home)
    def _():
        kept.start()

    @pl.when(jnp.logical_not(at_home))
    def _():
        outgoing(0, me).start()

    copies = []

    def answer(slot, owner):
        part_out[slot] = mixed(gated_in[slot])
        copy = outgoing(slot, owner)
        copy.start()
        copies.append(copy)

    for hop in hops:
        slot = 2 * hop
        gathers[slot].wait_recv()
        gathers[slot + 1] = gather(gated_in.at[slot], slot + 1, partner)
        answer(slot, 2 * lax.rem(place - hop + far, far) + side)
    for hop in [0] + hops:
        slot = 2 * hop + 1
        gathers[slot].wait_recv()
        answer(slot, 2 * lax.rem(place - hop + far, far) + 1 - side)

    for which in range(each):
        total = None
        for other in range(groups):
            slot = which * groups + other
            pltpu.make_async_copy(part_out.at[0], part_in.at[slot], part_recv.at[slot]).wait()
            term = part_in[slot].astype(jnp.float32)
            total = term if total is None else total + term
        out_ref[:, which * width : (which + 1) * width] = total.astype(jnp.bfloat16)
    for copy in list(gathers.values()) + copies:
        copy.wait_send()

    @pl.when(jnp.logical_not(at_home))
    def _():
        outgoing(0, me).wait_send()


def mix(gated_rows, w_mix):
    ways, groups = lax.axis_size("kv"), lax.axis_size("tp")
    count, rows = gated_rows.shape
    width = w_mix.shape[1]
    vmem = pl.BlockSpec(memory_space=pltpu.VMEM)
    dma = pltpu.SemaphoreType.DMA((ways,))
    return pl.pallas_call(
        functools.partial(mix_kernel, ways, groups),
        out_shape=jax.ShapeDtypeStruct((count, ways // groups * width), jnp.bfloat16),
        in_specs=[vmem] * 2,
        out_specs=vmem,
        scratch_shapes=[
            pltpu.VMEM((ways, count, rows), jnp.bfloat16),
            pltpu.VMEM((ways, count, width), jnp.bfloat16),
            pltpu.VMEM((ways, count, width), jnp.bfloat16),
        ]
        + [dma] * 4,
        compiler_params=pltpu.CompilerParams(collective_id=1, has_side_effects=True),
    )(gated_rows, w_mix)


def project_by_digits(flat_rows, norm_gain, weights, w_mix):
    token_count, model_width = flat_rows.shape
    shard_rows = weights[0].shape[0]
    own = lax.axis_index("kv")
    kv_bits = lax.axis_size("kv").bit_length() - 1
    near_bits = kv_bits // 2
    near = 2**near_bits
    far = lax.axis_size("kv") // near
    digit_shape = (2,) * near_bits
    collected = collect_digits(
        weights + (w_mix,),
        (0, 0, 0, 0, 0, 1),
        own,
        range(near_bits, kv_bits),
        lambda parts, bit: jax.tree.map(
            lambda part, own: part.astype(own.dtype),
            from_partner(shortened(parts), "kv", bit),
            parts,
        ),
    )
    far_mix = collected[5]
    token_digits = jnp.moveaxis(flat_rows.reshape(token_count, far, near, shard_rows), 2, 0)
    token_digits = token_digits.reshape(digit_shape + (token_count, far, shard_rows))
    arrived = butterfly(
        token_digits, own, near_bits, lambda part, bit: from_partner(part, "kv", bit)
    )
    gathered = arrived.reshape(near * token_count, far * shard_rows)
    gain_part = lax.dynamic_index_in_dim(
        norm_gain.reshape(far, near, shard_rows), own % near, 1, keepdims=False
    ).reshape(far * shard_rows)
    widened = gathered.astype(jnp.float32)
    scaled_in = (widened * gain_part).astype(jnp.bfloat16)
    partials = tuple(
        (
            jnp.dot(scaled_in, weight, preferred_element_type=jnp.float32).reshape(
                digit_shape + (token_count, weight.shape[1])
            )
            for weight in collected[:5]
        )
    )
    part_squares = jnp.sum(widened * widened, axis=-1).reshape(digit_shape + (token_count,))
    summed = halving(
        partials + (part_squares,),
        own,
        near_bits,
        lambda parts, bit: jax.tree.map(
            lambda part, own: part.astype(own.dtype),
            from_partner(shortened(parts), "kv", bit),
            parts,
        ),
    )
    totals = summed[:5]
    sum_squares = summed[5]
    row_scale = lax.rsqrt(sum_squares / model_width + epsilon)[:, None]
    return (
        tuple((total * row_scale).astype(jnp.bfloat16) for total in totals[:4]),
        totals[4] * row_scale,
        far_mix,
    )


def mix_by_digits(gated_rows, far_mix, model_width):
    token_count = gated_rows.shape[0]
    shard_rows = model_width // lax.axis_size("kv")
    own = lax.axis_index("kv")
    kv_bits = lax.axis_size("kv").bit_length() - 1
    near_bits = kv_bits // 2
    near = 2**near_bits
    far = lax.axis_size("kv") // near
    digit_shape = (2,) * near_bits
    near_gated = collect_digits(
        (gated_rows,),
        (0,),
        own,
        range(near_bits),
        lambda parts, bit: jax.tree.map(
            lambda part, own: part.astype(own.dtype),
            from_partner(shortened(parts), "kv", bit),
            parts,
        ),
    )[0]
    group_part = jnp.dot(near_gated, far_mix, preferred_element_type=jnp.float32).astype(
        jnp.bfloat16
    )
    group_part = group_part.reshape(digit_shape + (token_count, far, shard_rows))
    placed = butterfly(group_part, own, near_bits, lambda part, bit: from_partner(part, "kv", bit))
    placed = placed.reshape(near, token_count, far, shard_rows).transpose(1, 2, 0, 3)
    partial_out = placed.reshape(token_count, model_width).astype(jnp.float32)
    mixed_out = lax.psum_scatter(
        partial_out.astype(jnp.bfloat16), "tp", scatter_dimension=1, tiled=True
    )
    return mixed_out


def shards(
    tokens,
    norm_gain,
    w_query,
    w_key,
    w_value,
    w_outgate,
    w_gates,
    forget_bias,
    head_gain,
    w_mix,
    state_cell,
    state_norm,
    state_max,
    pend_keys,
    pend_values,
    pend_gates,
    accepted,
):
    sequences, proposals, model_width = tokens.shape
    token_count = sequences * proposals
    local_heads = forget_bias.shape[0]
    head_size = state_cell.shape[-1]
    shard_rows = w_query.shape[0]
    weights = (w_query, w_key, w_value, w_outgate)
    flat_gates = w_gates.reshape(shard_rows, -1)
    flat_rows = tokens.reshape(token_count, model_width)
    direct = (
        shard_rows % 128 == 0
        and w_mix.shape[1] % 128 == 0
        and lax.axis_size("kv") % 2 == 0
        and lax.axis_size("kv") % lax.axis_size("tp") == 0
    )
    if direct:
        columns, gate_pre = project(flat_rows, norm_gain, weights, flat_gates)
        queries, new_keys, new_values, outgate = jnp.split(columns, len(weights), axis=1)
    else:
        projected, gate_pre, far_mix = project_by_digits(
            flat_rows, norm_gain, weights + (flat_gates,), w_mix
        )
        queries, new_keys, new_values, outgate = projected
    gate_pre = gate_pre.reshape(sequences, proposals, 2, local_heads)

    def split_heads(array):
        return array.astype(jnp.float32).reshape(sequences, proposals, local_heads, head_size)

    key_scale = head_size ** (-0.5)
    cell_new, norm_new, new_max = fold_pending(
        state_cell,
        state_norm,
        state_max,
        split_heads(pend_keys) * key_scale,
        split_heads(pend_values),
        pend_gates,
        forget_bias,
        accepted,
    )
    log_in = gate_pre[:, :, 0, :]
    log_keep = jax.nn.log_sigmoid(gate_pre[:, :, 1, :] + forget_bias)
    hidden = read_block(
        split_heads(queries),
        split_heads(new_keys) * key_scale,
        split_heads(new_values),
        log_in,
        log_keep,
        cell_new,
        norm_new,
        new_max,
    )
    normed = hidden * lax.rsqrt(jnp.mean(hidden * hidden, axis=-1, keepdims=True) + epsilon)
    normed = normed * head_gain.reshape(local_heads, head_size)
    gated_rows = (jax.nn.sigmoid(split_heads(outgate)) * normed).astype(jnp.bfloat16)
    gated_rows = gated_rows.reshape(token_count, local_heads * head_size)
    if direct:
        mixed_out = mix(gated_rows, w_mix)
    else:
        mixed_out = mix_by_digits(gated_rows, far_mix, model_width)
    return (mixed_out.reshape(sequences, proposals, -1), cell_new, norm_new, new_max)


def solution(mesh):
    return jax.shard_map(
        shards,
        mesh=mesh,
        in_specs=(
            P("kv", None, None),
            P(),
            P("kv", "tp"),
            P("kv", "tp"),
            P("kv", "tp"),
            P("kv", "tp"),
            P("kv", None, "tp"),
            P("tp"),
            P("tp"),
            P("tp", "kv"),
            P("kv", "tp", None, None),
            P("kv", "tp", None),
            P("kv", "tp"),
            P("kv", None, "tp"),
            P("kv", None, "tp"),
            P("kv", None, None, "tp"),
            P("kv"),
        ),
        out_specs=(
            P("kv", None, "tp"),
            P("kv", "tp", None, None),
            P("kv", "tp", None),
            P("kv", "tp"),
        ),
        check_vma=False,
    )
```
